128 devices in a mesh: sp: 32 (over z, y, core), tp: 4 (over x).
Axes of the slice: x: 4, y: 4, z: 4, core: 2. Of those that a mesh axis runs over, the one named last changes fastest.
Arguments:
- stream: bfloat16 [8192, 2048], P('sp', 'tp'), may hold values from -1200 to 1200, as said below
- mix_gain: bfloat16 [2048], P('tp'), may hold values from 0.099609375 to 1.8984375
- pool_weight: bfloat16 [4, 512, 512], P('tp'), may hold values from -0.25 to 0.25
- pool_scale: bfloat16 [2048], P('tp'), may hold values from 0.099609375 to 1.8984375
- ffn_gain: bfloat16 [2048], replicated, may hold values from 0.099609375 to 1.8984375
- routes: int32 [8192, 2], P(('sp', 'tp')), may hold values from 0 to 31, all different within a row; in each aligned block of 64 rows (0 to 63, 64 to 127, ...) at most 8 rows name the same one
- route_weight: float32 [8192, 2], P(('sp', 'tp')), may hold values from 0.1 to 1
- w_gate: bfloat16 [32, 2048, 7168], P('sp', None, 'tp'), may hold values from -0.125 to 0.125
- w_up: bfloat16 [32, 2048, 7168], P('sp', None, 'tp'), may hold values from -0.125 to 0.125
- w_down: bfloat16 [32, 7168, 2048], P('sp', 'tp'), may hold values from -0.0625 to 0.0625
Outputs:
- layer_out: bfloat16 [8192, 2048], P(('sp', 'tp'))
The draws below stay inside these ranges and needn't reach their ends.
Inputs may be any that keep to these rules, and one draw needn't show every extreme that they name: `routes`: each row names 2 different experts. Within each aligned block of 64 rows (the rows of one device) no expert is named by more than 8 rows, a bound that some block reaches. `stream`: finite values.
All inputs are finite; a program needn't handle non-finite values.
Results may differ from the reference program's by a relative error of at most 0.0061.
Values may be sent and summed in bfloat16 or wider, within the bound.
A program may use at most 128 MiB of HBM per device.

```python
import math
import jax
import jax.numpy as jnp
import numpy as np
from jax import lax

D = 2048
GROUPS = 4
FF = 7168
TOP = 2
GROUP_W = 512
TQ = 64
EXPERTS = 32
CAP = 8
TOKENS = 8192
N_SP = 32
N_TP = 4


def draw_stream(key, part):
    key_base = jax.random.fold_in(key, 11)
    key_cols = jax.random.fold_in(key, 12)
    base_draw = jnp.clip(jax.random.normal(key_base, (TOKENS, D), jnp.float32), -6.0, 6.0)
    col_scale = jnp.exp(jax.random.uniform(key_cols, (D,), jnp.float32) * math.log(10.0))
    group_index = (jnp.arange(D) // (D // GROUPS)).astype(jnp.float32)
    rise = 3.0 ** (group_index / (GROUPS - 1))
    values = base_draw / 8.0
    return (values * col_scale * rise).astype(jnp.bfloat16)


def block_scale(rng, extent, split, least, top_value):
    level = 1.0
    for dim, blocks in split:
        heights = jax.random.uniform(jax.random.fold_in(jax.random.fold_in(rng, 6), dim), (blocks,), jnp.float32, least / len(split), top_value / len(split))
        level = level * jnp.repeat(jnp.exp(heights), extent[dim] // blocks).reshape((-1,) + (1,) * (len(extent) - 1 - dim))
    return level


def deal_out(stream_key, own, number, rows, amount, top, bound, slope):
    ranking = jax.random.permutation(stream_key, amount)
    heavy_load, usual = portions_of(amount, rows * top, bound, slope, True), portions_of(amount, rows * top, bound, slope, False)
    places = jnp.arange(amount)

    def named(sizes, turn):
        used = int((sizes > 0).sum())
        fixed = max(1, used // 4)
        passed = fixed + (places - fixed + turn * (used - fixed)) % max(1, amount - fixed)
        return jnp.zeros((amount,), jnp.int32).at[ranking[jnp.where(places < fixed, places, passed)]].set(jnp.asarray(sizes, jnp.int32))

    sizes = jnp.where(number % 4 == 0, named(heavy_load, number // 4), named(usual, number - number // 4 - 1))
    mixed = jax.random.permutation(jax.random.fold_in(own, 3), amount)
    donor, receiver = mixed[0:amount // 2 * 2:2], mixed[1:amount // 2 * 2:2]
    slack = jnp.minimum(sizes[donor] - 1, bound - sizes[receiver]) // 2
    slack = jnp.where((donor == ranking[0]) | (receiver == ranking[0]) | (sizes[receiver] == 0), 0, jnp.maximum(slack, 0))
    passed = jax.random.randint(jax.random.fold_in(own, 4), (amount // 2,), 0, 1 << 20) % (slack + 1)
    sizes = sizes.at[donor].add(-passed).at[receiver].add(passed)
    members = jnp.searchsorted(jnp.cumsum(sizes), jnp.arange(rows * top), side="right").astype(jnp.int32)
    table = members.reshape(top, rows).T
    table = table[jax.random.permutation(jax.random.fold_in(own, 1), rows)]
    turn = jax.random.randint(jax.random.fold_in(own, 2), (rows, 1), 0, top)
    return jnp.take_along_axis(table, (jnp.arange(top)[None, :] + turn) % top, axis=1)


def portions_of(amount, total, bound, skew, full):
    portions = [(1 << 20) // math.isqrt(rank ** skew) + 1 for rank in range(1, amount + 1)]
    largest = bound if full else min(bound, max(-(-total // amount), total * portions[0] // sum(portions)))
    least = 1 if total - largest >= amount - 1 else 0
    given, rest = [largest] + [least] * (amount - 1), total - largest - least * (amount - 1)
    while rest > 0:
        free = [i for i in range(1, amount) if given[i] < largest] or [i for i in range(1, amount) if given[i] < bound]
        mass, left = sum([portions[i] for i in free]), rest
        for i in free:
            extra = min(bound - given[i], max(1, left * portions[i] // mass), rest)
            given[i] = given[i] + extra
            rest = rest - extra
    return np.array(given)


def gaussian(key, extent, spread, bound, shards=(), held_as=jnp.bfloat16):
    drawn = jax.random.normal(key, extent, jnp.float32) * spread
    if len(shards) > 0:
        drawn = block_scale(key, extent, shards, -0.22, 0.18) * drawn
    return jnp.clip(drawn, min=-bound, max=bound).astype(held_as)


def setup_inputs(seed: int = 0) -> dict:
    seeds = jax.random.split(jax.random.key(seed), 11)
    stream = draw_stream(jax.random.fold_in(seeds[10], 71), 0)
    mix_gain = jnp.clip(1.0 + 0.18 * jax.random.normal(seeds[1], (D,), jnp.float32), 0.099609375, 1.8984375).astype(jnp.bfloat16)
    pool_weight = gaussian(seeds[2], (GROUPS, GROUP_W, GROUP_W), GROUP_W ** -0.5, 0.25, ((0, 4),))
    pool_scale = jnp.clip(1.0 + 0.18 * jax.random.normal(seeds[3], (D,), jnp.float32), 0.099609375, 1.8984375).astype(jnp.bfloat16)
    ffn_gain = jnp.clip(1.0 + 0.18 * jax.random.normal(seeds[4], (D,), jnp.float32), 0.099609375, 1.8984375).astype(jnp.bfloat16)
    routes_keys = jax.random.split(jax.random.fold_in(seeds[5], 1), TOKENS // TQ)
    routes_turns = jax.random.permutation(jax.random.fold_in(seeds[5], 3), TOKENS // TQ)
    routes = jax.vmap(lambda own, number: deal_out(jax.random.fold_in(seeds[5], 2), own, number, TQ, EXPERTS, TOP, CAP, 1))(routes_keys, routes_turns).reshape((TOKENS, TOP))
    route_weight = jnp.clip(0.1 + 0.9 * jax.random.uniform(seeds[6], (TOKENS, TOP), jnp.float32) ** block_scale(seeds[6], (TOKENS, TOP), ((0, 128),), -0.2, 0.2), 0.1, 1.0)
    w_gate = gaussian(seeds[7], (EXPERTS, D, FF), D ** -0.5, 0.125, ((0, 32), (2, 4)))
    w_up = gaussian(seeds[8], (EXPERTS, D, FF), D ** -0.5, 0.125, ((0, 32), (2, 4)))
    w_down = gaussian(seeds[9], (EXPERTS, FF, D), FF ** -0.5, 0.0625, ((0, 32), (1, 4)))
    return dict(stream=stream, mix_gain=mix_gain, pool_weight=pool_weight, pool_scale=pool_scale, ffn_gain=ffn_gain, routes=routes, route_weight=route_weight, w_gate=w_gate, w_up=w_up, w_down=w_down)


NORM_EPS = 1e-06

def rms_norm(values, gain):
    row_scale = lax.rsqrt(lax.optimization_barrier(jnp.mean(values * values, axis=-1, keepdims=True)) + NORM_EPS)
    return (values * row_scale * gain.astype(jnp.float32)).astype(jnp.bfloat16)

def reference(stream, mix_gain, pool_weight, pool_scale, ffn_gain, routes, route_weight, w_gate, w_up, w_down):
    stream_f32 = stream.astype(jnp.float32)
    normed = rms_norm(stream_f32, mix_gain)
    normed_f32 = normed.astype(jnp.float32)
    group_width = D // GROUPS
    position = jnp.arange(1, TOKENS + 1).astype(jnp.float32)[:, None]
    group_outs = []
    for group_index in range(GROUPS):
        window_len = 2 ** (group_index + 1)
        columns = normed_f32[:, group_index * group_width:(group_index + 1) * group_width]
        window_sum = jnp.zeros_like(columns)
        for lag_rows in range(window_len):
            shifted = jnp.concatenate([jnp.zeros((lag_rows, group_width), jnp.float32), columns[:TOKENS - lag_rows]], axis=0)
            window_sum = window_sum + shifted
        pooled = (window_sum / jnp.minimum(position, jnp.float32(window_len)) - columns).astype(jnp.bfloat16)
        group_outs.append(jnp.dot(pooled, pool_weight[group_index], preferred_element_type=jnp.float32))
    mixer_out = jnp.concatenate(group_outs, axis=1) * pool_scale.astype(jnp.float32)
    after_mix = (stream_f32 + mixer_out).astype(jnp.bfloat16)
    after_f32 = after_mix.astype(jnp.float32)
    normed2 = rms_norm(after_f32, ffn_gain)
    flat_routes = routes.reshape(-1)
    flat_weight = route_weight.reshape(-1)
    max_rows = N_SP * N_TP * CAP
    ff_shard = FF // N_TP

    def one_expert(layer_sum, expert):
        chosen = flat_routes == expert
        picked = jnp.nonzero(chosen, size=max_rows, fill_value=0)[0].astype(jnp.int32)
        is_valid = (jnp.arange(max_rows) < jnp.sum(chosen.astype(jnp.int32))).astype(jnp.float32)
        token_index = picked // TOP
        expert_rows = normed2[token_index]
        gate_val = jnp.dot(expert_rows, w_gate[expert], preferred_element_type=jnp.float32)
        up_val = jnp.dot(expert_rows, w_up[expert], preferred_element_type=jnp.float32)
        hidden = (jax.nn.silu(gate_val) * up_val).astype(jnp.bfloat16)
        summed = jnp.zeros((max_rows, D), jnp.float32)
        for shard_index in range(N_TP):
            block_out = jnp.dot(hidden[:, shard_index * ff_shard:(shard_index + 1) * ff_shard], w_down[expert, shard_index * ff_shard:(shard_index + 1) * ff_shard], preferred_element_type=jnp.float32).astype(jnp.bfloat16)
            summed = summed + lax.optimization_barrier(block_out).astype(jnp.float32)
        expert_out = lax.optimization_barrier(summed.astype(jnp.bfloat16)).astype(jnp.float32)
        weight = flat_weight[picked] * is_valid
        layer_sum = layer_sum.at[token_index].add(weight[:, None] * expert_out)
        return (layer_sum, None)
    expert_total, unused = lax.scan(one_expert, jnp.zeros((TOKENS, D), jnp.float32), jnp.arange(EXPERTS).astype(jnp.int32))
    return (after_f32 + expert_total).astype(jnp.bfloat16)
```

```python
import functools

import jax
import jax.numpy as jnp
from jax import lax
from jax.experimental import pallas as pl
from jax.experimental.pallas import tpu as pltpu
from jax.sharding import PartitionSpec as P

NORM_EPS = 1e-06
MESH = pl.DeviceIdType.MESH
STEPS = (0, 1, 3, 2)
CHUNKS = 4
PEERS = 8
TILE = 256


def split_up(array, dim, count):
    before, after = (array.shape[:dim], array.shape[dim + 1 :])
    return jnp.moveaxis(array.reshape(*before, count, -1, *after), dim, 0)


def sent_to_all(array, axis):
    copies = jnp.broadcast_to(array, (lax.axis_size(axis), *array.shape))
    return lax.all_to_all(copies, axis, split_axis=0, concat_axis=0, tiled=True)


def of_everyone(array, axis):
    return sent_to_all(array, axis).sum(axis=0)


def passed_along(block, axis, distance):
    devices = range(lax.axis_size(axis))
    route = [(i - distance, i) for i in devices if i - distance in devices]
    return lax.ppermute(block, axis, route)


def relative_place(expert, sp):
    dz = (expert // 8 - sp // 8 + 4) % 4
    dy = (expert // 2 % 4 - sp // 2 % 4 + 4) % 4
    dc = (expert + sp) % 2
    def place(d):
        return jnp.where(d == 2, 3, jnp.where(d == 3, 2, d))
    return place(dz) * PEERS + place(dy) * 2 + dc


def experts_kernel(
    s_ref, wg_hbm, wu_hbm, wd_hbm, r_ref,
    x_buf, wg, wu, wd, hid, part, relay_l, relay_r, from_l, from_r, sums,
    w_sem, d_ssem, d_rsem, g_ssem, g_rsem, p_ssem, p_rsem, r_ssem, r_rsem,
):
    sp = lax.axis_index("sp")
    tp = lax.axis_index("tp")
    z, y, core = sp // 8, sp // 2 % 4, sp % 2
    left, right = (sp, (tp + 3) % 4), (sp, (tp + 1) % 4)
    width = wd.shape[0] * TILE
    up_tiles, down_tiles = wg.shape[0], wd.shape[0]

    w_up_copies, w_down_copies = [], []
    for j in range(up_tiles):
        cols = pl.ds(j * TILE, TILE)
        for i, (src, dst) in enumerate(((wg_hbm, wg), (wu_hbm, wu))):
            w_up_copies.append(
                pltpu.make_async_copy(src.at[0, :, cols], dst.at[j], w_sem.at[2 * j + i])
            )
    for j in range(down_tiles):
        w_down_copies.append(
            pltpu.make_async_copy(
                wd_hbm.at[0, :, pl.ds(j * TILE, TILE)], wd.at[j], w_sem.at[2 * up_tiles + j]
            )
        )

    barrier = pltpu.get_barrier_semaphore()

    def peer(k, sign):
        dz, dy, dc = STEPS[k // PEERS], STEPS[k % PEERS // 2], k % 2
        if sign < 0:
            dz, dy = (4 - dz) % 4, (4 - dy) % 4
        return (((z + dz) % 4) * 8 + ((y + dy) % 4) * 2 + (core + dc) % 2, tp)

    for k in range(1, CHUNKS * PEERS):
        pl.semaphore_signal(barrier, inc=1, device_id=peer(k, 1), device_id_type=MESH)
    for neighbour in (left, right):
        pl.semaphore_signal(barrier, inc=1, device_id=neighbour, device_id_type=MESH)
    for copy in w_up_copies + w_down_copies:
        copy.start()
    pl.semaphore_wait(barrier, CHUNKS * PEERS + 1)

    def remote(src, dst, ssem, rsem, target):
        return pltpu.make_async_remote_copy(
            src_ref=src, dst_ref=dst, send_sem=ssem, recv_sem=rsem,
            device_id=target, device_id_type=MESH,
        )

    sent = []
    dispatch = {}
    for k in range(1, CHUNKS * PEERS):
        dispatch[k] = remote(
            s_ref.at[k], x_buf.at[k // PEERS, 0, k % PEERS], d_ssem.at[k], d_rsem.at[k], peer(k, 1)
        )
        dispatch[k].start()
        sent.append(dispatch[k])
    x_buf[0, 0, 0] = s_ref[0]

    def arrived(c):
        for k in range(c * PEERS, (c + 1) * PEERS):
            if k:
                dispatch[k].wait_recv()

    shared = {}

    def share(c):
        shared[c] = (
            remote(x_buf.at[c, 0, pl.ds(0, 4)], x_buf.at[c, 1, pl.ds(0, 4)],
                   g_ssem.at[c, 0], g_rsem.at[c, 0], left),
            remote(x_buf.at[c, 0, pl.ds(4, 4)], x_buf.at[c, 1, pl.ds(4, 4)],
                   g_ssem.at[c, 1], g_rsem.at[c, 1], right),
        )
        for copy in shared[c]:
            copy.start()
            sent.append(copy)

    def up(c):
        for copy in shared[c]:
            copy.wait_recv()
        if c == 0:
            for copy in w_up_copies:
                copy.wait()

        def tile(j, carry):
            rows = x_buf[c].reshape(2 * PEERS * 16, width)
            gate = jnp.dot(rows, wg[j], preferred_element_type=jnp.float32)
            raised = jnp.dot(rows, wu[j], preferred_element_type=jnp.float32)
            hid[j] = (jax.nn.silu(gate) * raised).astype(jnp.bfloat16)
            return carry

        lax.fori_loop(0, up_tiles, tile, 0)

    def down(c):
        if c == 0:
            for copy in w_down_copies:
                copy.wait()

        def tile(j, carry):
            rows = jnp.concatenate([hid[i] for i in range(up_tiles)], axis=1)
            out = jnp.dot(rows, wd[j], preferred_element_type=jnp.float32)
            out = out.reshape(2, PEERS, 2, 8, TILE)
            own, other = out[0], out[1]
            cols = pl.ds(pl.multiple_of(j * TILE, TILE), TILE)
            blocks = (
                own[:, 0],
                own[:, 1],
                jnp.concatenate([other[:4, 0], other[4:, 1]], axis=0),
                jnp.concatenate([other[:4, 1], other[4:, 0]], axis=0),
            )
            for b, block in enumerate(blocks):
                part[c, b, :, cols] = block.reshape(PEERS * 8, TILE).astype(jnp.bfloat16)
            return carry

        lax.fori_loop(0, down_tiles, tile, 0)

    head, tail = pl.ds(0, 32), pl.ds(32, 32)
    moves = {}

    def reduce_first(c):
        moves[c] = [
            remote(part.at[c, 1, head], relay_l.at[c], p_ssem.at[c, 0], p_rsem.at[c, 0], right),
            remote(part.at[c, 1, tail], relay_r.at[c], p_ssem.at[c, 1], p_rsem.at[c, 1], left),
            remote(part.at[c, 2, tail], from_l.at[c, tail], p_ssem.at[c, 2], p_rsem.at[c, 2], right),
            remote(part.at[c, 3, head], from_r.at[c, head], p_ssem.at[c, 3], p_rsem.at[c, 3], left),
            remote(part.at[c, 2, head], from_l.at[c, head], p_ssem.at[c, 4], p_rsem.at[c, 4], right),
            remote(part.at[c, 3, tail], from_r.at[c, tail], p_ssem.at[c, 5], p_rsem.at[c, 5], left),
        ]
        for copy in moves[c][:4]:
            copy.start()
        sent.extend(moves[c])

    def reduce_second(c):
        moves[c][0].wait_recv()
        moves[c][1].wait_recv()

        def tile(j, carry):
            cols = pl.ds(pl.multiple_of(j * TILE, TILE), TILE)
            for b, rows, relay in ((2, head, relay_l), (3, tail, relay_r)):
                total = part[c, b, rows, cols].astype(jnp.float32) + relay[c, :, cols].astype(
                    jnp.float32
                )
                part[c, b, rows, cols] = total.astype(jnp.bfloat16)
            return carry

        lax.fori_loop(0, down_tiles, tile, 0)
        moves[c][4].start()
        moves[c][5].start()

    returns = {}

    def reduce_third(c):
        for copy in moves[c][2:]:
            copy.wait_recv()

        def tile(j, carry):
            cols = pl.ds(pl.multiple_of(j * TILE, TILE), TILE)
            total = (
                part[c, 0, :, cols].astype(jnp.float32)
                + from_l[c, :, cols].astype(jnp.float32)
                + from_r[c, :, cols].astype(jnp.float32)
            )
            sums[c, :, :, cols] = total.reshape(PEERS, 8, TILE).astype(jnp.bfloat16)
            return carry

        lax.fori_loop(0, down_tiles, tile, 0)
        for i in range(PEERS):
            k = c * PEERS + i
            if k:
                returns[k] = remote(
                    sums.at[c, i], r_ref.at[k], r_ssem.at[k], r_rsem.at[k], peer(k, -1)
                )
                returns[k].start()
                sent.append(returns[k])
            else:
                r_ref[0] = sums[0, 0]

    for c in range(2):
        arrived(c)
        share(c)
    for c in range(CHUNKS):
        up(c)
        if c + 2 < CHUNKS:
            arrived(c + 2)
            share(c + 2)
        if c:
            reduce_second(c - 1)
        down(c)
        reduce_first(c)
        if c:
            reduce_third(c - 1)
    reduce_second(CHUNKS - 1)
    reduce_third(CHUNKS - 1)
    for k in range(1, CHUNKS * PEERS):
        returns[k].wait_recv()
    for copy in sent:
        copy.wait_send()


def run_experts(send_rows, w_gate, w_up, w_down):
    width, inner = w_gate.shape[1:]
    up_tiles, down_tiles = inner // TILE, width // TILE
    bf16 = jnp.bfloat16
    dma = pltpu.SemaphoreType.DMA
    count = CHUNKS * PEERS
    return pl.pallas_call(
        experts_kernel,
        name="experts",
        out_shape=jax.ShapeDtypeStruct((count, 8, width), bf16),
        in_specs=[pl.BlockSpec(memory_space=pltpu.VMEM)] + [pl.BlockSpec(memory_space=pl.ANY)] * 3,
        out_specs=pl.BlockSpec(memory_space=pltpu.VMEM),
        scratch_shapes=[
            pltpu.VMEM((CHUNKS, 2, PEERS, 16, width), bf16),
            pltpu.VMEM((up_tiles, width, TILE), bf16),
            pltpu.VMEM((up_tiles, width, TILE), bf16),
            pltpu.VMEM((down_tiles, inner, TILE), bf16),
            pltpu.VMEM((up_tiles, 2 * PEERS * 16, TILE), bf16),
            pltpu.VMEM((CHUNKS, 4, PEERS * 8, width), bf16),
            pltpu.VMEM((CHUNKS, PEERS * 4, width), bf16),
            pltpu.VMEM((CHUNKS, PEERS * 4, width), bf16),
            pltpu.VMEM((CHUNKS, PEERS * 8, width), bf16),
            pltpu.VMEM((CHUNKS, PEERS * 8, width), bf16),
            pltpu.VMEM((CHUNKS, PEERS, 8, width), bf16),
            dma((2 * up_tiles + down_tiles,)),
            dma((count,)), dma((count,)),
            dma((CHUNKS, 2)), dma((CHUNKS, 2)),
            dma((CHUNKS, 6)), dma((CHUNKS, 6)),
            dma((count,)), dma((count,)),
        ],
        compiler_params=pltpu.CompilerParams(
            collective_id=0, has_side_effects=True, vmem_limit_bytes=60 * 2**20
        ),
    )(send_rows, w_gate, w_up, w_down)


def slots_of(routes, sp, sp_count, slots):
    flat = routes.reshape(-1)
    is_expert = (flat[:, None] == jnp.arange(sp_count, dtype=jnp.int32)[None, :]).astype(jnp.int32)
    rank = jnp.cumsum(is_expert, axis=0) - is_expert
    slot = jnp.sum(rank * is_expert, axis=1)
    return relative_place(flat, sp).reshape(routes.shape), slot.reshape(routes.shape)


def per_device(
    stream, mix_gain, pool_weight, pool_scale, ffn_gain, routes, route_weight, w_gate, w_up, w_down
):
    tok_rows, shard_width = stream.shape
    tp_count = lax.axis_size("tp")
    sp_count = lax.axis_size("sp")
    sp = lax.axis_index("sp")
    model_width = shard_width * tp_count
    across = [(i, (i + 2) % tp_count) for i in range(tp_count)]
    routes_across = lax.ppermute(routes, "tp", across)
    stream_f32 = stream.astype(jnp.float32)
    square = of_everyone(jnp.sum(stream_f32 * stream_f32, axis=1), "tp")
    row_scale = lax.rsqrt(square / model_width + NORM_EPS)[:, None]
    normed = (stream_f32 * row_scale * mix_gain.astype(jnp.float32)).astype(jnp.bfloat16)
    local_groups = pool_weight.shape[0]
    halo_rows = 2 ** (local_groups * tp_count) - 1
    previous = passed_along(normed[tok_rows - halo_rows :], "sp", 1)
    extended = jnp.concatenate([previous, normed], axis=0)
    first_row = sp * tok_rows
    position = first_row + jnp.arange(tok_rows, dtype=jnp.int32)
    source = first_row - halo_rows + jnp.arange(tok_rows + halo_rows, dtype=jnp.int32)
    lag_rows = position[:, None] - source[None, :]
    group_index = lax.axis_index("tp") * local_groups + 0
    window_len = jnp.left_shift(jnp.int32(2), group_index)
    band_mask = ((lag_rows >= 0) & (lag_rows < window_len)).astype(jnp.bfloat16)
    window_sum = jnp.dot(band_mask, extended, preferred_element_type=jnp.float32)
    window_count = jnp.minimum(position + 1, window_len).astype(jnp.float32)[:, None]
    own_rows = normed.astype(jnp.float32)
    pooled = (window_sum / window_count - own_rows).astype(jnp.bfloat16)
    group_outs = jnp.dot(pooled, pool_weight[0], preferred_element_type=jnp.float32)
    mixer_out = group_outs * pool_scale.astype(jnp.float32)
    after_mix = (stream_f32 + mixer_out).astype(jnp.bfloat16)
    block_rows = tok_rows // tp_count
    blocks = after_mix.reshape(tp_count, block_rows, shard_width)
    doubled = jnp.stack([blocks, jnp.roll(blocks, -2, axis=0)], axis=1)
    taken = lax.all_to_all(doubled, "tp", split_axis=0, concat_axis=0, tiled=True)
    taken = taken.transpose(1, 2, 0, 3).reshape(2 * block_rows, model_width)
    after_f32 = taken.astype(jnp.float32)
    ffn_scale = lax.rsqrt(jnp.mean(after_f32 * after_f32, axis=1, keepdims=True) + NORM_EPS)
    normed2 = (after_f32 * ffn_scale * ffn_gain.astype(jnp.float32)).astype(jnp.bfloat16)
    tok_count, top_count = routes.shape
    capacity = 2 * tok_count * top_count // sp_count
    own_place, own_slot = slots_of(routes, sp, sp_count, capacity)
    far_place, far_slot = slots_of(routes_across, sp, sp_count, capacity)
    send_ids = jnp.arange(sp_count * 2 * capacity, dtype=jnp.int32)

    def mask_of(place, slot, offset):
        target = place * (2 * capacity) + offset + slot
        hits = target[None, :, :] == send_ids[:, None, None]
        return hits.any(axis=2).astype(jnp.bfloat16)

    dispatch_mask = jnp.concatenate(
        [mask_of(own_place, own_slot, 0), mask_of(far_place, far_slot, capacity)], axis=1
    )
    send_rows = jnp.dot(dispatch_mask, normed2, preferred_element_type=jnp.float32).astype(
        jnp.bfloat16
    )
    send_rows = send_rows.reshape(sp_count, 2 * capacity, model_width)
    returned = run_experts(send_rows, w_gate, w_up, w_down).reshape(
        sp_count * capacity, model_width
    )
    slot_ids = jnp.arange(sp_count * capacity, dtype=jnp.int32)
    dest = own_place * capacity + own_slot
    expert_sum = after_f32[:block_rows]
    for pick_index in range(top_count):
        pick = (dest[:, pick_index][:, None] == slot_ids[None, :]).astype(jnp.bfloat16)
        picked_out = jnp.dot(pick, returned, preferred_element_type=jnp.float32)
        expert_sum = expert_sum + route_weight[:, pick_index : pick_index + 1] * picked_out
    return expert_sum.astype(jnp.bfloat16)


def solution(mesh):
    in_specs = (
        P("sp", "tp"),
        P("tp"),
        P("tp", None, None),
        P("tp"),
        P(),
        P(("sp", "tp"), None),
        P(("sp", "tp"), None),
        P("sp", None, "tp"),
        P("sp", None, "tp"),
        P("sp", "tp", None),
    )
    out_specs = P(("sp", "tp"), None)
    return jax.shard_map(
        per_device, mesh=mesh, in_specs=in_specs, out_specs=out_specs, check_vma=False
    )
```

```python
import functools

import jax
import jax.numpy as jnp
from jax import lax
from jax.experimental import pallas as pl
from jax.experimental.pallas import tpu as pltpu
from jax.sharding import PartitionSpec as P

NORM_EPS = 1e-06
MESH = pl.DeviceIdType.MESH
F32, BF16 = jnp.float32, jnp.bfloat16
COMBOS = (
    (0, 0), (0, 1),
    (0, 3), (1, 0), (3, 0), (1, 1),
    (3, 3), (1, 3), (3, 1), (0, 2),
    (2, 0), (1, 2), (2, 1), (3, 2),
    (2, 3), (2, 2),
)
ORDER = tuple((dz, dy, dc) for dz, dy in COMBOS for dc in (0, 1))
PEERS = len(ORDER)
CHUNKS = (4, 8, 8, 8, 4)
BASES = tuple(sum(CHUNKS[:c]) for c in range(len(CHUNKS)))
LAST = len(CHUNKS) - 1
CAP = 8
UP, DOWN, COLS = 896, 512, 512


def layer_kernel(
    stream_hbm, mix_gain_hbm, pool_weight_hbm, pool_scale_hbm, ffn_gain_hbm,
    routes_hbm, weights_hbm, wg_hbm, wu_hbm, wd_hbm,
    out_ref,
    stream, mix_gain, pool_weight, pool_scale, ffn_gain, routes, weights, far_routes,
    row_sums, peer_sums, edge_sums, edge_rows, mixed, taken, picks, back, send,
    own, other, wg, wu, wd, hid, part, relay_l, relay_r, from_l, from_r, sums, returned,
    in_sem, w_sem, f_ssem, f_rsem, m_ssem, m_rsem, d_ssem, d_rsem,
    g_ssem, g_rsem, p_ssem, p_rsem, r_ssem, r_rsem,
):
    sp = lax.axis_index("sp")
    tp = lax.axis_index("tp")
    z, y, core = sp // 8, sp // 2 % 4, sp % 2
    left, right, far = (sp, (tp + 3) % 4), (sp, (tp + 1) % 4), (sp, (tp + 2) % 4)
    onward, behind = (sp + 1) % PEERS, (sp + PEERS - 1) % PEERS
    tok_rows, group = stream.shape
    block_rows = tok_rows // 4
    width = out_ref.shape[1]
    up_tiles, down_tiles = wg.shape[0], wd.shape[0]

    def peer_sp(k, sign):
        dz, dy, dc = ORDER[k]
        if sign < 0:
            dz, dy = (4 - dz) % 4, (4 - dy) % 4
        return ((z + dz) % 4) * 8 + ((y + dy) % 4) * 2 + (core + dc) % 2

    barrier = pltpu.get_barrier_semaphore()
    greeted = [(peer_sp(k, 1), tp) for k in range(1, PEERS)] + [left, right, far]
    greeted += [(s, (tp + d) % 4) for s in (onward, behind) for d in (1, 2, 3)]
    for target in greeted:
        pl.semaphore_signal(barrier, inc=1, device_id=target, device_id_type=MESH)

    loads = [
        pltpu.make_async_copy(src, dst, in_sem.at[i])
        for i, (src, dst) in enumerate(
            (
                (stream_hbm, stream), (routes_hbm, routes), (weights_hbm, weights),
                (mix_gain_hbm, mix_gain), (pool_scale_hbm, pool_scale), (ffn_gain_hbm, ffn_gain),
                (pool_weight_hbm, pool_weight),
            )
        )
    ]
    for copy in loads:
        copy.start()
    w_up_copies = [
        pltpu.make_async_copy(
            src.at[0, :, pl.ds(j * UP, UP)], dst.at[j], w_sem.at[2 * j + i]
        )
        for j in range(up_tiles)
        for i, (src, dst) in enumerate(((wg_hbm, wg), (wu_hbm, wu)))
    ]
    w_down_copies = [
        pltpu.make_async_copy(
            wd_hbm.at[0, :, pl.ds(j * DOWN, DOWN)], wd.at[j], w_sem.at[2 * up_tiles + j]
        )
        for j in range(down_tiles)
    ]
    for copy in w_up_copies + w_down_copies:
        copy.start()

    sent = []

    def remote(src, dst, ssem, rsem, target):
        copy = pltpu.make_async_remote_copy(
            src_ref=src, dst_ref=dst, send_sem=ssem, recv_sem=rsem,
            device_id=target, device_id_type=MESH,
        )
        sent.append(copy)
        return copy

    for copy in loads[:3]:
        copy.wait()
    square = stream[...].astype(F32)
    square = square * square
    high = square.astype(BF16)
    low = (square - high.astype(F32)).astype(BF16)
    ones = jnp.ones((8, group), BF16)
    lanes = (((1,), (1,)), ((), ()))
    row_sums[...] = lax.dot_general(
        ones, high, lanes, preferred_element_type=F32
    ) + lax.dot_general(ones, low, lanes, preferred_element_type=F32)

    pl.semaphore_wait(barrier, len(greeted))

    edge = remote(
        stream.at[pl.ds(tok_rows - 16, 16)], edge_rows, f_ssem.at[7], f_rsem.at[7], (onward, tp)
    )
    spread = [
        remote(row_sums, peer_sums.at[d - 1], f_ssem.at[d - 1], f_rsem.at[d - 1], (sp, (tp + d) % 4))
        for d in (1, 2, 3)
    ]
    edge_spread = [
        remote(
            row_sums.at[:, pl.ds(tok_rows - 128, 128)], edge_sums.at[d],
            f_ssem.at[3 + d], f_rsem.at[3 + d], (onward, (tp + d) % 4),
        )
        for d in range(4)
    ]
    swap = remote(routes, far_routes, f_ssem.at[8], f_rsem.at[8], far)
    for copy in spread + edge_spread + [edge, swap]:
        copy.start()
    for copy in loads[3:]:
        copy.wait()

    position = lax.broadcasted_iota(jnp.int32, (tok_rows, 1), 0)
    window = jnp.left_shift(jnp.int32(2), tp)
    lag = position - lax.broadcasted_iota(jnp.int32, (tok_rows, tok_rows), 1)
    band = jnp.where((lag >= 0) & (lag < window), 1.0, 0.0).astype(BF16)
    edge_lag = position[:16] + 16 - lax.broadcasted_iota(jnp.int32, (16, 16), 1)
    edge_limit = jnp.where(sp == 0, 0, window)
    edge_band = jnp.where(edge_lag < edge_limit, 1.0, 0.0).astype(BF16)
    count = jnp.minimum(position + sp * tok_rows + 1, window).astype(F32)

    def row_scale(total):
        scale = lax.rsqrt(total[0:1] / width + NORM_EPS)
        return jnp.broadcast_to(scale, (128, total.shape[1])).T[:, 0:1]

    gain = mix_gain[...].reshape(1, group).astype(F32)
    for copy in spread:
        copy.wait_recv()
    total = row_sums[...] + peer_sums[0] + peer_sums[1] + peer_sums[2]
    normed = (stream[...].astype(F32) * row_scale(total) * gain).astype(BF16)
    window_sum = jnp.dot(band, normed, preferred_element_type=F32)
    for copy in edge_spread + [edge]:
        copy.wait_recv()
    edge_total = edge_sums[0] + edge_sums[1] + edge_sums[2] + edge_sums[3]
    edge_normed = (edge_rows[...].astype(F32) * row_scale(edge_total)[112:] * gain).astype(BF16)
    first = window_sum[:16] + jnp.dot(edge_band, edge_normed, preferred_element_type=F32)
    window_sum = jnp.concatenate([first, window_sum[16:]], axis=0)
    pooled = (window_sum / count - normed.astype(F32)).astype(BF16)
    grouped = jnp.dot(pooled, pool_weight[0], preferred_element_type=F32)
    grouped = grouped * pool_scale[...].reshape(1, group).astype(F32)
    after = (stream[...].astype(F32) + grouped).astype(BF16)
    mixed[...] = after.reshape(4, block_rows, group)

    exchange = []
    for d in (2, 1, 3):
        to = (tp + d) % 4
        for j in range(2):
            exchange.append(
                remote(
                    mixed.at[(to + 2 * j) % 4], taken.at[tp, j],
                    m_ssem.at[d - 1, j], m_rsem.at[d - 1, j], (sp, to),
                )
            )
            exchange[-1].start()
    for j in range(2):
        taken[tp, j] = mixed[(tp + 2 * j) % 4]

    swap.wait_recv()
    lane = lax.broadcasted_iota(jnp.int32, (1, 128), 1)
    first_route, second_route = (
        jnp.concatenate([routes[i : i + 1], far_routes[i : i + 1]], axis=1) for i in range(2)
    )
    weight = jnp.concatenate([weights[...], jnp.zeros((2, 64), F32)], axis=1)
    row = lax.broadcasted_iota(jnp.int32, (PEERS, 128), 0)
    expert = jnp.zeros((PEERS, 128), jnp.int32)
    for k in range(PEERS):
        expert = jnp.where(row == k, peer_sp(k, 1), expert)
    is_first = jnp.where(expert == first_route, 1.0, 0.0)
    is_second = jnp.where(expert == second_route, 1.0, 0.0)
    named = is_first + is_second
    before = lax.broadcasted_iota(jnp.int32, (128, 128), 0)
    token = lax.broadcasted_iota(jnp.int32, (128, 128), 1)
    earlier = jnp.where((before < token) & (before // 64 == token // 64), 1.0, 0.0).astype(BF16)
    rank = jnp.dot(named.astype(BF16), earlier, preferred_element_type=F32)
    slot = jnp.where(named > 0.0, rank + jnp.where(lane >= 64, 8.0, 0.0), -1.0)
    share_of = is_first * weight[0:1] + is_second * weight[1:2]
    slots16 = lax.broadcasted_iota(jnp.int32, (16, 128), 0).astype(F32)
    for k in range(PEERS):
        hit = slot[k : k + 1] == slots16
        picks[k * 16 : (k + 1) * 16] = jnp.where(hit, 1.0, 0.0).astype(BF16)
        back[k * 8 : (k + 1) * 8] = jnp.where(hit[:8], share_of[k : k + 1], 0.0)

    for copy in exchange:
        copy.wait_recv()

    squares = jnp.zeros((2 * block_rows, 1), F32)
    for g in range(4):
        rows = taken[g].reshape(2 * block_rows, group).astype(F32)
        squares = squares + jnp.sum(rows * rows, axis=1, keepdims=True)
    ffn_scale = lax.rsqrt(squares / width + NORM_EPS)
    ffn_gain_row = ffn_gain[...].reshape(1, width).astype(F32)
    for g in range(4):
        cols = pl.ds(g * group, group)
        rows = taken[g].reshape(2 * block_rows, group).astype(F32)
        rows = (rows * ffn_scale * ffn_gain_row[:, g * group : (g + 1) * group]).astype(BF16)
        picked = jnp.dot(picks[...], rows, preferred_element_type=F32)
        send[:, :, cols] = picked.reshape(PEERS, 16, group).astype(BF16)

    dispatch = {}
    for k in range(1, PEERS):
        dispatch[k] = remote(
            send.at[k], own.at[k], d_ssem.at[k], d_rsem.at[k], (peer_sp(k, 1), tp)
        )
        dispatch[k].start()
    own[0] = send[0]

    def arrived(c):
        for k in range(BASES[c], BASES[c] + CHUNKS[c]):
            if k:
                dispatch[k].wait_recv()

    shared = {}

    def share(c):
        half = CHUNKS[c] // 2
        shared[c] = []
        for i, target in enumerate((left, right)):
            places = pl.ds(BASES[c] + i * half, half)
            shared[c].append(
                remote(own.at[places], other.at[places], g_ssem.at[c, i], g_rsem.at[c, i], target)
            )
            shared[c][-1].start()

    def up(c):
        for copy in shared[c]:
            copy.wait_recv()
        if c == 0:
            for copy in w_up_copies:
                copy.wait()
        n, places = CHUNKS[c], pl.ds(BASES[c], CHUNKS[c])

        def tile(j, carry):
            rows = jnp.concatenate(
                [own[places].reshape(n * 16, width), other[places].reshape(n * 16, width)], axis=0
            )
            gate = jnp.dot(rows, wg[j], preferred_element_type=F32)
            raised = jnp.dot(rows, wu[j], preferred_element_type=F32)
            hid[j, : n * 32] = (jax.nn.silu(gate) * raised).astype(BF16)
            return carry

        lax.fori_loop(0, up_tiles, tile, 0)

    def down(c):
        if c == 0:
            for copy in w_down_copies:
                copy.wait()
        n, half = CHUNKS[c], CHUNKS[c] // 2
        span = pl.ds(BASES[c] * CAP, n * CAP)

        def tile(j, carry):
            rows = jnp.concatenate([hid[i, : n * 32] for i in range(up_tiles)], axis=1)
            out = jnp.dot(rows, wd[j], preferred_element_type=F32)
            out = out.reshape(2, n, 2, CAP, DOWN)
            mine, others = out[0], out[1]
            cols = pl.ds(pl.multiple_of(j * DOWN, DOWN), DOWN)
            blocks = (
                mine[:, 0],
                mine[:, 1],
                jnp.concatenate([others[:half, 0], others[half:, 1]], axis=0),
                jnp.concatenate([others[:half, 1], others[half:, 0]], axis=0),
            )
            for b, block in enumerate(blocks):
                part[b, span, cols] = block.reshape(n * CAP, DOWN).astype(BF16)
            return carry

        lax.fori_loop(0, down_tiles, tile, 0)

    moves = {}

    def halves(c):
        half = CHUNKS[c] // 2 * CAP
        base = BASES[c] * CAP
        return pl.ds(base, half), pl.ds(base + half, half), pl.ds(base // 2, half)

    def reduce_first(c):
        head, tail, via = halves(c)
        plan = (
            (1, head, relay_l, via, right),
            (1, tail, relay_r, via, left),
            (2, tail, from_l, tail, right),
            (3, head, from_r, head, left),
            (2, head, from_l, head, right),
            (3, tail, from_r, tail, left),
        )
        moves[c] = [
            remote(part.at[b, src], buffer.at[dst], p_ssem.at[c, i], p_rsem.at[c, i], target)
            for i, (b, src, buffer, dst, target) in enumerate(plan)
        ]
        for copy in moves[c][:4]:
            copy.start()

    def reduce_second(c):
        head, tail, via = halves(c)
        moves[c][0].wait_recv()
        moves[c][1].wait_recv()
        for j in range(width // COLS):
            cols = pl.ds(j * COLS, COLS)
            for b, rows, relay in ((2, head, relay_l), (3, tail, relay_r)):
                total = part[b, rows, cols].astype(F32) + relay[via, cols].astype(F32)
                part[b, rows, cols] = total.astype(BF16)
        moves[c][4].start()
        moves[c][5].start()

    returns = {}

    def reduce_third(c):
        for copy in moves[c][2:]:
            copy.wait_recv()
        n = CHUNKS[c]
        span, places = pl.ds(BASES[c] * CAP, n * CAP), pl.ds(BASES[c], n)
        for j in range(width // COLS):
            cols = pl.ds(j * COLS, COLS)
            total = part[0, span, cols].astype(F32) + from_l[span, cols].astype(F32)
            total = total + from_r[span, cols].astype(F32)
            sums[places, :, cols] = total.reshape(n, CAP, COLS).astype(BF16)
        for k in range(BASES[c], BASES[c] + n):
            if k:
                returns[k] = remote(
                    sums.at[k], returned.at[pl.ds(k * CAP, CAP)],
                    r_ssem.at[k], r_rsem.at[k], (peer_sp(k, -1), tp),
                )
                returns[k].start()
            else:
                returned[0:CAP] = sums[0]

    for c in range(2):
        arrived(c)
        share(c)
    spread_weight = back[...].T[:block_rows]
    weight_high = spread_weight.astype(BF16)
    weight_low = (spread_weight - weight_high.astype(F32)).astype(BF16)
    combine = jnp.concatenate([weight_high, weight_low], axis=0)
    picks[: 2 * block_rows] = combine[:, :128]
    picks[2 * block_rows : 4 * block_rows] = combine[:, 128:]
    for c in range(len(CHUNKS)):
        up(c)
        if c + 2 < len(CHUNKS):
            arrived(c + 2)
            share(c + 2)
        if c:
            reduce_second(c - 1)
        down(c)
        reduce_first(c)
        if c:
            reduce_third(c - 1)
    reduce_second(LAST)
    reduce_third(LAST)
    for k in range(1, PEERS):
        returns[k].wait_recv()
    combine = jnp.concatenate(
        [picks[: 2 * block_rows], picks[2 * block_rows : 4 * block_rows]], axis=1
    )
    for g in range(4):
        cols = pl.ds(g * group, group)
        gained = jnp.dot(combine, returned[:, cols], preferred_element_type=F32)
        gained = gained[:block_rows] + gained[block_rows:]
        out_ref[:, cols] = (taken[g, 0].astype(F32) + gained).astype(BF16)
    for copy in sent:
        copy.wait_send()


def per_device(
    stream, mix_gain, pool_weight, pool_scale, ffn_gain, routes, route_weight, w_gate, w_up, w_down
):
    tok_rows, group = stream.shape
    width, inner = w_gate.shape[1:]
    block_rows = tok_rows // 4
    up_tiles, down_tiles = inner // UP, width // DOWN
    dma = pltpu.SemaphoreType.DMA
    slots = PEERS * CAP
    return pl.pallas_call(
        layer_kernel,
        name="experts",
        out_shape=jax.ShapeDtypeStruct((block_rows, width), BF16),
        in_specs=[pl.BlockSpec(memory_space=pltpu.HBM)] * 10,
        out_specs=pl.BlockSpec(memory_space=pltpu.VMEM),
        scratch_shapes=[
            pltpu.VMEM((tok_rows, group), BF16),
            pltpu.VMEM((group,), BF16),
            pltpu.VMEM((1, group, group), BF16),
            pltpu.VMEM((group,), BF16),
            pltpu.VMEM((width,), BF16),
            pltpu.VMEM((2, block_rows), jnp.int32),
            pltpu.VMEM((2, block_rows), F32),
            pltpu.VMEM((2, block_rows), jnp.int32),
            pltpu.VMEM((8, tok_rows), F32),
            pltpu.VMEM((3, 8, tok_rows), F32),
            pltpu.VMEM((4, 8, 128), F32),
            pltpu.VMEM((16, group), BF16),
            pltpu.VMEM((4, block_rows, group), BF16),
            pltpu.VMEM((4, 2, block_rows, group), BF16),
            pltpu.VMEM((PEERS * 16, 128), BF16),
            pltpu.VMEM((slots, 128), F32),
            pltpu.VMEM((PEERS, 16, width), BF16),
            pltpu.VMEM((PEERS, 16, width), BF16),
            pltpu.VMEM((PEERS, 16, width), BF16),
            pltpu.VMEM((up_tiles, width, UP), BF16),
            pltpu.VMEM((up_tiles, width, UP), BF16),
            pltpu.VMEM((down_tiles, inner, DOWN), BF16),
            pltpu.VMEM((up_tiles, max(CHUNKS) * 32, UP), BF16),
            pltpu.VMEM((4, slots, width), BF16),
            pltpu.VMEM((slots // 2, width), BF16),
            pltpu.VMEM((slots // 2, width), BF16),
            pltpu.VMEM((slots, width), BF16),
            pltpu.VMEM((slots, width), BF16),
            pltpu.VMEM((PEERS, CAP, width), BF16),
            pltpu.VMEM((slots, width), BF16),
            dma((7,)),
            dma((2 * up_tiles + down_tiles,)),
            dma((9,)), dma((9,)),
            dma((3, 2)), dma((3, 2)),
            dma((PEERS,)), dma((PEERS,)),
            dma((len(CHUNKS), 2)), dma((len(CHUNKS), 2)),
            dma((len(CHUNKS), 6)), dma((len(CHUNKS), 6)),
            dma((PEERS,)), dma((PEERS,)),
        ],
        compiler_params=pltpu.CompilerParams(
            collective_id=0, has_side_effects=True, vmem_limit_bytes=62 * 2**20
        ),
    )(
        stream, mix_gain, pool_weight, pool_scale, ffn_gain,
        routes.T, route_weight.T, w_gate, w_up, w_down,
    )


def solution(mesh):
    in_specs = (
        P("sp", "tp"),
        P("tp"),
        P("tp", None, None),
        P("tp"),
        P(),
        P(("sp", "tp"), None),
        P(("sp", "tp"), None),
        P("sp", None, "tp"),
        P("sp", None, "tp"),
        P("sp", "tp", None),
    )
    out_specs = P(("sp", "tp"), None)
    return jax.shard_map(
        per_device, mesh=mesh, in_specs=in_specs, out_specs=out_specs, check_vma=False
    )
```
